512 devices in a mesh: sp: 64 (over z, y), tp: 8 (over x, core).
Axes of the slice: x: 4, y: 4, z: 16, core: 2. Of those that a mesh axis runs over, the one named last changes fastest.
Arguments:
- latent: bfloat16 [16384, 2048], P(('sp', 'tp')), may hold values from -3 to 3
- context: bfloat16 [1024, 2048], P('sp'), may hold values from -6 to 6
- condition: float32 [2048], replicated, may hold values from -6 to 6
- ctx_cond: float32 [2048], replicated, may hold values from -6 to 6
- norm_gain: float32 [2048], replicated, may hold values from 0.1 to 1.9
- w_shift: bfloat16 [2048, 2048], P('sp', 'tp'), may hold values from -0.25 to 0.25
- w_scale: bfloat16 [2048, 2048], P('sp', 'tp'), may hold values from -0.25 to 0.25
- w_gate: bfloat16 [2048, 2048], P('sp', 'tp'), may hold values from -0.25 to 0.25
- w_query: bfloat16 [2048, 2048], P(None, 'tp'), may hold values from -0.125 to 0.125
- w_key: bfloat16 [2048, 2048], P(None, 'tp'), may hold values from -0.125 to 0.125
- w_value: bfloat16 [2048, 2048], P(None, 'tp'), may hold values from -0.125 to 0.125
- w_out: bfloat16 [2048, 2048], P('tp'), may hold values from -0.125 to 0.125
- rel_bias: float32 [16, 15, 31], replicated, may hold values from 2 to 250
Outputs:
- updated: bfloat16 [16384, 2048], P(('sp', 'tp'))
The draws below stay inside these ranges and needn't reach their ends.
All inputs are finite; a program needn't handle non-finite values.
Results may differ from the reference program's by a relative error of at most 0.015.
Values may be sent and summed in bfloat16 or wider, within the bound.
No kernel may reach another device: no remote copies, remote signals or barrier semaphores. Data moves between devices by JAX's collectives and lax.ppermute only.
A program may use at most 64 MiB of HBM per device.

```python
import jax
import jax.numpy as jnp
import numpy as np
from jax import lax

D = 2048
HEADS = 16
HEAD_DIM = 128
GRID_W = 32
WIN_H = 8
WIN_W = 16
CTX = 1024
TOKENS = 16384
N_TP = 8


def draw_rel_bias(key, part):
    drawn = jax.random.uniform(key, (HEADS, 2 * WIN_H - 1, 2 * WIN_W - 1), jnp.float32, 2.0, 4.0)
    return drawn


def steps_of(stream_key, dims, split, low, largest):
    loudness, own = 1.0, jax.random.fold_in(stream_key, 6)
    for axis_at, blocks in split:
        steps = jnp.exp(jax.random.uniform(jax.random.fold_in(own, axis_at), (blocks,), jnp.float32, low / len(split), largest / len(split)))
        loudness = loudness * jnp.repeat(steps, dims[axis_at] // blocks).reshape([-1 if axis == axis_at else 1 for axis in range(len(dims))])
    return loudness


def noise(own_key, dims, deviation, limit, shards=(), held_as=jnp.bfloat16):
    level = steps_of(own_key, dims, shards, -0.22, 0.18) if shards else 1.0
    values = jax.random.normal(own_key, dims, jnp.float32) * deviation * level
    return jnp.minimum(jnp.maximum(values, -limit), limit).astype(held_as)


def setup_inputs(seed: int = 0) -> dict:
    splits = jax.random.split(jax.random.key(seed), 14)
    return {
        "latent": noise(splits[0], (TOKENS, D), 0.5, 3.0, ((0, 512),)),
        "context": noise(splits[1], (CTX, D), 1.0, 6.0, ((0, 64),)),
        "condition": noise(splits[2], (D,), 1.0, 6.0, (), jnp.float32),
        "ctx_cond": noise(splits[3], (D,), 1.0, 6.0, (), jnp.float32),
        "norm_gain": jnp.clip(1.0 + 0.18 * jax.random.normal(splits[4], (D,), jnp.float32), 0.1, 1.9),
        "w_shift": noise(splits[5], (D, D), (D // 4) ** -0.5, 0.25, ((0, 64), (1, 8))),
        "w_scale": noise(splits[6], (D, D), (D // 4) ** -0.5, 0.25, ((0, 64), (1, 8))),
        "w_gate": noise(splits[7], (D, D), (D // 4) ** -0.5, 0.25, ((0, 64), (1, 8))),
        "w_query": noise(splits[8], (D, D), D ** -0.5, 0.125, ((1, 8),)),
        "w_key": noise(splits[9], (D, D), D ** -0.5, 0.125, ((1, 8),)),
        "w_value": noise(splits[10], (D, D), D ** -0.5, 0.125, ((1, 8),)),
        "w_out": noise(splits[11], (D, D), D ** -0.5, 0.125, ((0, 8),)),
        "rel_bias": draw_rel_bias(jax.random.fold_in(splits[13], 71), 0),
    }


NORM_EPS = 1e-06
NEG_BIG = -1e+30

def rms_mod(block, norm_gain, shifts, scales):
    block = block.astype(jnp.float32)
    normed = block * lax.rsqrt(lax.optimization_barrier(jnp.mean(block * block, axis=-1, keepdims=True)) + NORM_EPS) * norm_gain
    return (normed * (1.0 + scales) + shifts).astype(jnp.bfloat16)

def project(block, weight):
    return jnp.dot(block, weight, preferred_element_type=jnp.float32).astype(jnp.bfloat16)

def geometry(total_rows):
    row_ids = np.arange(total_rows)
    starts = np.clip(row_ids - WIN_H // 2, 0, total_rows - WIN_H)
    row_index = starts[:, None] + np.arange(WIN_H)[None, :]
    row_off = row_index - row_ids[:, None] + WIN_H - 1
    col_ids = np.arange(GRID_W)
    col_start = np.clip(col_ids - WIN_W // 2, 0, GRID_W - WIN_W)
    col_in = (col_ids[None, :] >= col_start[:, None]) & (col_ids[None, :] < col_start[:, None] + WIN_W)
    col_off = np.clip(col_ids[None, :] - col_ids[:, None], 1 - WIN_W, WIN_W - 1) + WIN_W - 1
    return (row_index, row_off, col_in, col_off)

def reference(latent, context, condition, ctx_cond, norm_gain, w_shift, w_scale, w_gate, w_query, w_key, w_value, w_out, rel_bias):
    activated = jax.nn.silu(jnp.stack([condition, ctx_cond])).astype(jnp.bfloat16)
    shifts = jnp.dot(activated, w_shift, preferred_element_type=jnp.float32)
    scales = jnp.dot(activated, w_scale, preferred_element_type=jnp.float32)
    gate_vec = jnp.dot(activated[:1], w_gate, preferred_element_type=jnp.float32)[0]
    normed = rms_mod(latent, norm_gain, shifts[0], scales[0])
    ctx_normed = rms_mod(context, norm_gain, shifts[1], scales[1])
    queries = project(normed, w_query)
    lat_keys = project(normed, w_key)
    lat_values = project(normed, w_value)
    ctx_keys = project(ctx_normed, w_key)
    ctx_values = project(ctx_normed, w_value)
    total_rows = latent.shape[0] // GRID_W
    row_index, row_off, col_in, col_off = geometry(total_rows)
    inv_scale = HEAD_DIM ** (-0.5)

    def grid_heads(array):
        return jnp.transpose(array.reshape(total_rows, GRID_W, HEADS, HEAD_DIM), (2, 0, 1, 3))

    def ctx_heads(array):
        return jnp.transpose(array.reshape(-1, HEADS, HEAD_DIM), (1, 0, 2))

    def per_head(operands):
        query_head, key_head, value_head, ctx_key_head, ctx_value_head, bias_table = operands
        query_f = query_head.astype(jnp.float32)
        key_win = key_head[row_index].astype(jnp.float32)
        val_win = value_head[row_index].astype(jnp.float32)
        bias_win = bias_table[row_off[:, None, :, None], col_off[None, :, None, :]]
        scores_win = jnp.einsum('rqd,rkwd->rqkw', query_f, key_win) * inv_scale + bias_win
        scores_win = jnp.where(col_in[None, :, None, :], scores_win, NEG_BIG)
        scores_ctx = jnp.einsum('rqd,cd->rqc', query_f, ctx_key_head.astype(jnp.float32)) * inv_scale
        row_max = jnp.maximum(lax.optimization_barrier(jnp.max(scores_win, axis=(2, 3))), lax.optimization_barrier(jnp.max(scores_ctx, axis=2)))
        exp_win = jnp.exp(scores_win - row_max[:, :, None, None])
        exp_ctx = jnp.exp(scores_ctx - row_max[:, :, None])
        row_total = lax.optimization_barrier(jnp.sum(exp_win, axis=(2, 3))) + lax.optimization_barrier(jnp.sum(exp_ctx, axis=2))
        probs_win = (exp_win / row_total[:, :, None, None]).astype(jnp.bfloat16)
        probs_ctx = (exp_ctx / row_total[:, :, None]).astype(jnp.bfloat16)
        mixed_head = jnp.einsum('rqkw,rkwd->rqd', probs_win.astype(jnp.float32), val_win)
        mixed_head = mixed_head + jnp.einsum('rqc,cd->rqd', probs_ctx.astype(jnp.float32), ctx_value_head.astype(jnp.float32))
        return mixed_head.astype(jnp.bfloat16)
    attended = lax.map(per_head, (grid_heads(queries), grid_heads(lat_keys), grid_heads(lat_values), ctx_heads(ctx_keys), ctx_heads(ctx_values), rel_bias))
    attended = jnp.transpose(attended, (1, 2, 0, 3)).reshape(-1, HEADS * HEAD_DIM)
    head_cols = HEADS // N_TP * HEAD_DIM
    branch = jnp.zeros(latent.shape, jnp.float32)
    for group_idx in range(N_TP):
        low = group_idx * head_cols
        part_sum = jnp.dot(attended[:, low:low + head_cols], w_out[low:low + head_cols], preferred_element_type=jnp.float32).astype(jnp.bfloat16)
        part_sum = lax.optimization_barrier(part_sum)
        branch = branch + part_sum.astype(jnp.float32)
    return (latent.astype(jnp.float32) + gate_vec * branch).astype(jnp.bfloat16)
```

```python
import functools

import jax
import jax.numpy as jnp
from jax import lax
from jax.experimental import pallas as pl
from jax.experimental.pallas import tpu as pltpu
from jax.sharding import Mesh
from jax.sharding import PartitionSpec as P

HEADS = 16
HEAD_DIM = 128
GRID_W = 32
WIN_H = 8
WIN_W = 16
D = 2048
SP = ("z", "y")
TP = ("x", "c")
ALL = ("z", "y", "x", "c")
NORM_EPS = 1e-06
NEG_BIG = -1e30
BF = jnp.bfloat16
F32 = jnp.float32


def call(body, outs, name, scratch=(), flops=0, vmem=None):
    return pl.pallas_call(
        body,
        out_shape=outs,
        scratch_shapes=list(scratch),
        name=name,
        cost_estimate=pl.CostEstimate(flops=flops, bytes_accessed=0, transcendentals=0),
        compiler_params=pltpu.CompilerParams(vmem_limit_bytes=vmem),
    )


def shape(dims, dtype):
    return jax.ShapeDtypeStruct(dims, dtype)


def mod_partial_body(cond_ref, ctxc_ref, wsh_ref, wsc_ref, wg_ref, out_ref, pad_ref):
    sp = lax.axis_index("z") * 4 + lax.axis_index("y")
    row = sp // 4
    off = pl.multiple_of((sp % 4) * 32, 32)
    cond = cond_ref[pl.ds(row, 1), :]
    ctxc = ctxc_ref[pl.ds(row, 1), :]
    act = jnp.concatenate([cond, ctxc] * 4, axis=0)
    act = (act / (1.0 + jnp.exp(-act))).astype(BF)
    pad_ref[...] = jnp.zeros_like(pad_ref)
    pad_ref[pl.ds(off, 32), 0:256] = wsh_ref[...]
    pad_ref[pl.ds(off, 32), 256:512] = wsc_ref[...]
    pad_ref[pl.ds(off, 32), 512:768] = wg_ref[...]
    res = jnp.dot(act, pad_ref[...], preferred_element_type=F32)
    row5 = jnp.concatenate(
        [res[0:1, 0:256], res[1:2, 0:256], res[0:1, 256:512], res[1:2, 256:512], res[0:1, 512:768]],
        axis=1,
    )
    for i in range(out_ref.shape[0]):
        out_ref[i] = row5


def sum_bcast_body(in_ref, out_ref):
    total = jnp.sum(in_ref[...], axis=0)
    for i in range(out_ref.shape[0]):
        out_ref[i] = total


def mod_row(mod_ref, xc, kind):
    total = mod_ref[xc, :, kind * 256 : (kind + 1) * 256]
    for y in range(1, 4):
        total = total + mod_ref[y * 8 + xc, :, kind * 256 : (kind + 1) * 256]
    return total


def normalize(load, mod_ref, gain_ref, xn_ref, rows, which):
    x = load().astype(F32)
    inv = lax.rsqrt(jnp.mean(x * x, axis=-1, keepdims=True) + NORM_EPS)
    for xc in range(8):
        cols = slice(xc * 256, (xc + 1) * 256)
        gain = gain_ref[:, cols] * (1.0 + mod_row(mod_ref, xc, 2 + which))
        xn_ref[:, cols] = (x[:, cols] * inv * gain + mod_row(mod_ref, xc, which)).astype(BF)


def ctx_kv_body(ctx_ref, mod_ref, gain_ref, wk_ref, wv_ref, out_ref, xn_ref):
    normalize(lambda: ctx_ref[...], mod_ref, gain_ref, xn_ref, 16, 1)
    xn = xn_ref[...]
    k = jnp.dot(xn, wk_ref[...], preferred_element_type=F32).astype(BF)
    v = jnp.dot(xn, wv_ref[...], preferred_element_type=F32).astype(BF)
    for i in range(out_ref.shape[0]):
        out_ref[i, 0] = k
        out_ref[i, 1] = v


def qkv_body(
    lat_ref, mod_ref, gain_ref, wq_ref, wk_ref, wv_ref, q_ref, head_ref, tail_ref, gate_ref, xn_ref
):
    normalize(lambda: lat_ref[...].reshape(256, D), mod_ref, gain_ref, xn_ref, 256, 0)
    xn = xn_ref[...]
    k = jnp.dot(xn, wk_ref[...], preferred_element_type=F32).astype(BF)
    head_ref[0] = k[:128]
    tail_ref[0] = k[128:]
    v = jnp.dot(xn, wv_ref[...], preferred_element_type=F32).astype(BF)
    head_ref[1] = v[:128]
    tail_ref[1] = v[128:]
    q_ref[...] = jnp.dot(xn, wq_ref[...], preferred_element_type=F32).astype(BF)
    for xc in range(8):
        gate_ref[:, xc * 256 : (xc + 1) * 256] = mod_row(mod_ref, xc, 4)


def bias_body(rows_total, tab_ref, out_ref, exp_ref):
    sp = lax.axis_index("z") * 4 + lax.axis_index("y")
    tp = lax.axis_index("x") * 2 + lax.axis_index("c")
    first = sp * 8
    lane = lax.broadcasted_iota(jnp.int32, (32, 128), 1)
    col = lax.broadcasted_iota(jnp.int32, (32, 128), 0)
    key_col = lane % 32
    start = jnp.clip(col - WIN_W // 2, 0, GRID_W - WIN_W)
    col_in = (key_col >= start) & (key_col < start + WIN_W)
    quarter = lane // 32
    for h in range(2):
        tab = tab_ref[tp * 2 + h]
        for d in range(15):
            line = jnp.broadcast_to(tab[d : d + 1, :], (32, 128))
            for p in range(4):
                exp_ref[d, p] = pltpu.roll(line, (32 * p - 15) % 128, 1, stride=1, stride_axis=0)
        for r in range(8):
            a = jnp.clip(first + r - WIN_H // 2, 0, rows_total - WIN_H) - first + WIN_H // 2
            half = r // 4
            for s in range(3):
                seg = half + s
                block = jnp.full((32, 128), NEG_BIG, F32)
                for p in range(4):
                    k = seg * 4 + p
                    d = k - r + 3
                    if 0 <= d < 15:
                        ok = (k >= a) & (k < a + WIN_H)
                        block = jnp.where(
                            (quarter == p) & col_in & ok, exp_ref[d, p], block
                        )
                out_ref[h, half, s, (r % 4) * 32 : (r % 4) * 32 + 32, :] = block


def attend_body(q_ref, prev_ref, head_ref, tail_ref, next_ref, bias_ref, ctx_ref, out_ref):
    core = lax.axis_index("c")
    inv = HEAD_DIM**-0.5
    segs = (prev_ref, head_ref, tail_ref, next_ref)
    nt = (((1,), (1,)), ((), ()))
    for h in range(2):
        hc = slice(h * 128, (h + 1) * 128)
        kc = ctx_ref[:, 0, :, hc].reshape(1024, 128)
        vc = ctx_ref[:, 1, :, hc].reshape(1024, 128)
        for half in range(2):
            q = q_ref[half * 128 : (half + 1) * 128, hc]
            s_ctx = lax.dot_general(q, kc, nt, preferred_element_type=F32) * inv
            s_win = [
                lax.dot_general(q, segs[half + s][0, :, hc], nt, preferred_element_type=F32) * inv
                + bias_ref[h, half, s]
                for s in range(3)
            ]
            top = jnp.max(s_ctx, axis=-1, keepdims=True)
            peak = jnp.maximum(jnp.maximum(s_win[0], s_win[1]), s_win[2])
            top = jnp.maximum(top, jnp.max(peak, axis=-1, keepdims=True))
            e_ctx = jnp.exp(s_ctx - top)
            e_win = [jnp.exp(s - top) for s in s_win]
            total = jnp.sum(e_ctx, axis=-1, keepdims=True) + jnp.sum(
                e_win[0] + e_win[1] + e_win[2], axis=-1, keepdims=True
            )
            acc = jnp.dot(e_ctx.astype(BF), vc, preferred_element_type=F32)
            for s in range(3):
                acc = acc + jnp.dot(
                    e_win[s].astype(BF), segs[half + s][1, :, hc], preferred_element_type=F32
                )
            out = (acc / total).astype(BF)
            for i in range(4):
                block = half * 4 + i
                slot = jnp.where(core == block % 2, 0, 1)
                out_ref[slot, (block // 2) * 32 : (block // 2) * 32 + 32, hc] = out[
                    i * 32 : (i + 1) * 32
                ]


def out_proj_body(mine_ref, got_ref, w_ref, wp_ref, out_ref):
    res = jnp.dot(mine_ref[...], w_ref[...], preferred_element_type=F32)
    res = res + jnp.dot(got_ref[...], wp_ref[...], preferred_element_type=F32)
    out_ref[...] = res.astype(BF).reshape(4, 32, D)


def final_body(parts_ref, lat_ref, gate_ref, out_ref):
    branch = jnp.sum(parts_ref[...].astype(F32), axis=0)
    out_ref[...] = (lat_ref[...].astype(F32) + gate_ref[...] * branch).astype(BF)


def exchange(blocks, axes):
    return lax.all_to_all(blocks, axes, 0, 0, tiled=True)


def on_device(
    latent,
    context,
    condition,
    ctx_cond,
    norm_gain,
    w_shift,
    w_scale,
    w_gate,
    w_query,
    w_key,
    w_value,
    w_out,
    rel_bias,
):
    gain = norm_gain.reshape(1, D)
    part = call(
        mod_partial_body,
        shape((16, 1, 1280), F32),
        "mod_partial",
        [pltpu.VMEM((128, 768), BF)],
    )(condition.reshape(16, 128), ctx_cond.reshape(16, 128), w_shift, w_scale, w_gate)
    lat_all = exchange(jnp.broadcast_to(latent[None], (8, 32, D)), TP)
    got = exchange(part, "z")
    summed = call(sum_bcast_body, shape((32, 1, 1280), F32), "sum_bcast")(got)
    mod = exchange(summed, ("y", "x", "c"))

    ctx_kv = call(
        ctx_kv_body,
        shape((16, 2, 16, 256), BF),
        "ctx_kv",
        [pltpu.VMEM((16, D), BF)],
        flops=10**8,
    )(context, mod, gain, w_key, w_value)
    ctx_z = exchange(ctx_kv, "z")
    ctx_all = exchange(jnp.broadcast_to(ctx_z[None], (4, 16, 2, 16, 256)), "y")

    q, head, tail, gate = call(
        qkv_body,
        (
            shape((256, 256), BF),
            shape((2, 128, 256), BF),
            shape((2, 128, 256), BF),
            shape((1, D), F32),
        ),
        "qkv",
        [pltpu.VMEM((256, D), BF)],
        flops=10**9,
    )(lat_all, mod, gain, w_query, w_key, w_value)
    count = 64
    prev = lax.ppermute(tail, SP, [(i, i + 1) for i in range(count - 1)])
    nxt = lax.ppermute(head, SP, [(i + 1, i) for i in range(count - 1)])
    table = jnp.pad(rel_bias, ((0, 0), (0, 1), (0, 97)))
    bias = call(
        functools.partial(bias_body, 512),
        shape((2, 2, 3, 128, 128), F32),
        "bias",
        [pltpu.VMEM((15, 4, 32, 128), F32)],
        flops=10**8,
    )(table)
    att = call(attend_body, shape((2, 128, 256), BF), "attend", flops=10**9)(
        q, prev, head, tail, nxt, bias, ctx_all.reshape(64, 2, 16, 256)
    )
    swap = [(0, 1), (1, 0)]
    w_pair = lax.ppermute(w_out, "c", swap)
    other = lax.ppermute(att[1], "c", swap)
    parts = call(out_proj_body, shape((4, 32, D), BF), "out_proj", flops=10**9)(
        att[0], other, w_out, w_pair
    )
    arrived = exchange(parts, "x")
    return call(final_body, shape((32, D), BF), "final")(arrived, latent, gate)


def solution(mesh):
    torus = Mesh(mesh.devices.reshape(16, 4, 4, 2), ALL)
    return jax.shard_map(
        on_device,
        mesh=torus,
        in_specs=(
            P(ALL, None),
            P(SP, None),
            P(),
            P(),
            P(),
            P(SP, TP),
            P(SP, TP),
            P(SP, TP),
            P(None, TP),
            P(None, TP),
            P(None, TP),
            P(TP, None),
            P(),
        ),
        out_specs=P(ALL, None),
        check_vma=False,
    )
```

```python
import functools

import jax
import jax.numpy as jnp
from jax import lax
from jax.experimental import pallas as pl
from jax.experimental.pallas import tpu as pltpu
from jax.sharding import Mesh
from jax.sharding import PartitionSpec as P


HEAD_DIM = 128
GRID_W = 32
WIN_H = 8
WIN_W = 16
D = 2048
SP = ("z", "y")
TP = ("x", "c")
ALL = ("z", "y", "x", "c")
NORM_EPS = 1e-06
NEG_BIG = -1e30
BF = jnp.bfloat16
F32 = jnp.float32


VMEM_SPEC = pl.BlockSpec(memory_space=pltpu.VMEM)
HBM_SPEC = pl.BlockSpec(memory_space=pltpu.HBM)


def call(body, outs, scratch=(), flops=0, vmem=8 << 20, **specs):
    return pl.pallas_call(
        body,
        out_shape=outs,
        **specs,
        scratch_shapes=list(scratch),
        cost_estimate=pl.CostEstimate(flops=flops, bytes_accessed=0, transcendentals=0),
        compiler_params=pltpu.CompilerParams(vmem_limit_bytes=vmem),
    )


def shape(dims, dtype):
    return jax.ShapeDtypeStruct(dims, dtype)


def mod_partial_body(
    cond_hbm, ctxc_hbm, wsh_hbm, wsc_hbm, wg_hbm, ctx_hbm, out_ref, pad_ref, act_ref, ctx_ref, sems
):
    sp = lax.axis_index("z") * 4 + lax.axis_index("y")
    tp = lax.axis_index("x") * 2 + lax.axis_index("c")
    row = sp // 4
    off = pl.multiple_of((sp % 4) * 32, 32)
    zero = jnp.zeros((32, 768), BF)
    for i in range(4):
        pad_ref[i * 32 : (i + 1) * 32] = zero
    cols = pl.ds(pl.multiple_of(tp * 256, 256), 256)
    copies = [
        pltpu.make_async_copy(src, dst, sems.at[i])
        for i, (src, dst) in enumerate(
            (
                (cond_hbm, act_ref.at[0]),
                (ctxc_hbm, act_ref.at[1]),
                (wsh_hbm, pad_ref.at[pl.ds(off, 32), 0:256]),
                (wsc_hbm, pad_ref.at[pl.ds(off, 32), 256:512]),
                (wg_hbm, pad_ref.at[pl.ds(off, 32), 512:768]),
                (ctx_hbm.at[:, cols], ctx_ref),
            )
        )
    ]
    for copy in copies:
        copy.start()
    for copy in copies:
        copy.wait()
    cond = act_ref[0, pl.ds(row, 1), :]
    ctxc = act_ref[1, pl.ds(row, 1), :]
    act = jnp.concatenate([cond, ctxc] * 4, axis=0)
    act = (act / (1.0 + jnp.exp(-act))).astype(BF)
    res = jnp.dot(act, pad_ref[...], preferred_element_type=F32)
    rows = jnp.concatenate(
        [
            res[0:2, 0:256],
            res[0:2, 256:512],
            res[0:1, 512:768],
            jnp.zeros((3, 256), F32),
        ],
        axis=0,
    )
    high = rows.astype(BF)
    low = (rows - high.astype(F32)).astype(BF)
    packed = jnp.concatenate([high.astype(F32), low.astype(F32)], axis=0).astype(BF)
    ctx = ctx_ref[...]
    for i in range(out_ref.shape[0]):
        out_ref[i, 0:16] = ctx
        out_ref[i, 16:32] = packed


def relay_body(in_ref, mod_ref, ctx_ref):
    total = jnp.sum(in_ref[:, 16:32, :].astype(F32), axis=0)
    total = total[0:8] + total[8:16]
    for i in range(mod_ref.shape[0]):
        mod_ref[i] = total
    ctx_ref[...] = in_ref[:, 0:16, :].reshape(256, 256)


def mod_row(mod_ref, xc, kind):
    total = mod_ref[xc, kind : kind + 1, :]
    for y in range(1, 4):
        total = total + mod_ref[y * 8 + xc, kind : kind + 1, :]
    return total


def gather_x_body(own_ref, p1_ref, p2_ref, p3_ref, out_ref):
    x = lax.axis_index("x")
    for d, ref in enumerate((own_ref, p1_ref, p2_ref, p3_ref)):
        out_ref[lax.rem(x - d + 4, 4)] = ref[...]


def ctx_kv_body(mine_ref, theirs_ref, mod_ref, gain_ref, wk_ref, wv_ref, out_ref, xn_ref):
    core = lax.axis_index("c")
    blocks = [(ref, j, 2 * j + c) for j in range(4) for ref, c in ((mine_ref, core), (theirs_ref, 1 - core))]
    square = jnp.zeros((256, 256), F32)
    for ref, j, _ in blocks:
        x = ref[j].astype(F32)
        square = square + x * x
    inv = lax.rsqrt(jnp.sum(square, axis=-1, keepdims=True) * (1.0 / D) + NORM_EPS)
    for ref, j, xc in blocks:
        cols = pl.ds(pl.multiple_of(xc * 256, 256), 256)
        gain = gain_ref[:, cols] * (1.0 + mod_row(mod_ref, xc, 3))
        xn_ref[:, cols] = (ref[j].astype(F32) * inv * gain + mod_row(mod_ref, xc, 1)).astype(BF)
    xn = xn_ref[...]
    k = jnp.dot(xn, wk_ref[...], preferred_element_type=F32).astype(BF)
    v = jnp.dot(xn, wv_ref[...], preferred_element_type=F32).astype(BF)
    for i in range(out_ref.shape[0]):
        out_ref[i, 0] = k
        out_ref[i, 1] = v


def qkv_body(
    mine_ref, theirs_ref, mod_ref, gain_ref, wq_ref, wk_ref, wv_ref,
    q_ref, head_ref, tail_ref, gate_ref, xn_ref,
):
    core = lax.axis_index("c")
    gains = [gain_ref[:, i * 256 : (i + 1) * 256] * (1.0 + mod_row(mod_ref, i, 2)) for i in range(8)]
    shifts = [mod_row(mod_ref, i, 0) for i in range(8)]
    gain = jnp.concatenate(gains, axis=1)
    shift = jnp.concatenate(shifts, axis=1)
    for ref, c in ((mine_ref, core), (theirs_ref, 1 - core)):
        for j in range(4):
            x = ref[j].astype(F32)
            inv = lax.rsqrt(jnp.sum(x * x, axis=-1, keepdims=True) * (1.0 / D) + NORM_EPS)
            rows = pl.ds(pl.multiple_of((2 * j + c) * 32, 32), 32)
            xn_ref[rows, :] = (x * inv * gain + shift).astype(BF)
    xn = xn_ref[...]
    k = jnp.dot(xn, wk_ref[...], preferred_element_type=F32).astype(BF)
    head_ref[0] = k[:128]
    tail_ref[0] = k[128:]
    v = jnp.dot(xn, wv_ref[...], preferred_element_type=F32).astype(BF)
    head_ref[1] = v[:128]
    tail_ref[1] = v[128:]
    q_ref[...] = jnp.dot(xn, wq_ref[...], preferred_element_type=F32).astype(BF)
    for xc in range(8):
        gate_ref[:, xc * 256 : (xc + 1) * 256] = mod_row(mod_ref, xc, 4)


def bias_body(rows_total, tab_ref, out_ref, exp_ref):
    sp = lax.axis_index("z") * 4 + lax.axis_index("y")
    tp = lax.axis_index("x") * 2 + lax.axis_index("c")
    first = sp * 8
    lane = lax.broadcasted_iota(jnp.int32, (32, 128), 1)
    col = lax.broadcasted_iota(jnp.int32, (32, 128), 0)
    key_col = lane % 32
    start = jnp.clip(col - WIN_W // 2, 0, GRID_W - WIN_W)
    col_in = (key_col >= start) & (key_col < start + WIN_W)
    quarter = lane // 32
    for h in range(2):
        tab = tab_ref[tp * 2 + h]
        for d in range(15):
            line = jnp.broadcast_to(tab[d : d + 1, :], (32, 128))
            for p in range(4):
                exp_ref[d, p] = pltpu.roll(line, (32 * p - 15) % 128, 1, stride=1, stride_axis=0)
        for r in range(8):
            a = jnp.clip(first + r - WIN_H // 2, 0, rows_total - WIN_H) - first + WIN_H // 2
            half = r // 4
            for s in range(3):
                seg = half + s
                block = jnp.full((32, 128), NEG_BIG, F32)
                for p in range(4):
                    k = seg * 4 + p
                    d = k - r + 3
                    if 0 <= d < 15:
                        ok = (k >= a) & (k < a + WIN_H)
                        block = jnp.where(
                            (quarter == p) & col_in & ok, exp_ref[d, p], block
                        )
                out_ref[h, half, s, (r % 4) * 32 : (r % 4) * 32 + 32, :] = block


def attend_body(q_ref, prev_ref, head_ref, tail_ref, next_ref, bias_ref, ctx_ref, mine_ref, other_ref):
    core = lax.axis_index("c")
    inv = HEAD_DIM**-0.5
    segs = (prev_ref, head_ref, tail_ref, next_ref)
    nt = (((1,), (1,)), ((), ()))
    for h in range(2):
        hc = slice(h * 128, (h + 1) * 128)
        kc = ctx_ref[:, 0, :, hc].reshape(1024, 128)
        vc = ctx_ref[:, 1, :, hc].reshape(1024, 128)
        for half in range(2):
            q = q_ref[half * 128 : (half + 1) * 128, hc]
            s_ctx = lax.dot_general(q, kc, nt, preferred_element_type=F32) * inv
            s_win = [
                lax.dot_general(q, segs[half + s][0, :, hc], nt, preferred_element_type=F32) * inv
                + bias_ref[h, half, s]
                for s in range(3)
            ]
            top = jnp.max(s_ctx, axis=-1, keepdims=True)
            peak = jnp.maximum(jnp.maximum(s_win[0], s_win[1]), s_win[2])
            top = jnp.maximum(top, jnp.max(peak, axis=-1, keepdims=True))
            e_ctx = jnp.exp(s_ctx - top)
            e_win = [jnp.exp(s - top) for s in s_win]
            total = jnp.sum(e_ctx, axis=-1, keepdims=True) + jnp.sum(
                e_win[0] + e_win[1] + e_win[2], axis=-1, keepdims=True
            )
            acc = jnp.dot(e_ctx.astype(BF), vc, preferred_element_type=F32)
            for s in range(3):
                acc = acc + jnp.dot(
                    e_win[s].astype(BF), segs[half + s][1, :, hc], preferred_element_type=F32
                )
            out = (acc / total).astype(BF)
            for i in range(2):
                even = out[i * 64 : i * 64 + 32]
                odd = out[i * 64 + 32 : i * 64 + 64]
                rows = slice((half * 2 + i) * 32, (half * 2 + i + 1) * 32)
                mine_ref[rows, hc] = jnp.where(core == 0, even, odd)
                other_ref[rows, hc] = jnp.where(core == 0, odd, even)


def out_proj_body(mine_ref, got_ref, w_ref, wp_ref, out_ref):
    res = jnp.dot(mine_ref[...], w_ref[...], preferred_element_type=F32)
    res = res + jnp.dot(got_ref[...], wp_ref[...], preferred_element_type=F32)
    out_ref[...] = res.astype(BF).reshape(4, 32, D)


def final_body(parts_ref, lat_ref, gate_ref, out_ref):
    branch = jnp.sum(parts_ref[...].astype(F32), axis=0)
    out_ref[...] = (lat_ref[...].astype(F32) + gate_ref[...] * branch).astype(BF)


def exchange(blocks, axes):
    return lax.all_to_all(blocks, axes, 0, 0, tiled=True)


SWAP = [(0, 1), (1, 0)]


def along_x(own):
    parts = [own]
    for d in (1, 2, 3):
        parts.append(lax.ppermute(own, "x", [(i, (i + d) % 4) for i in range(4)]))
    return parts


def on_device(
    latent,
    context,
    condition,
    ctx_cond,
    norm_gain,
    w_shift,
    w_scale,
    w_gate,
    w_query,
    w_key,
    w_value,
    w_out,
    rel_bias,
):
    gain = norm_gain.reshape(1, D)
    part = call(
        mod_partial_body,
        shape((16, 32, 256), BF),
        [
            pltpu.VMEM((128, 768), BF),
            pltpu.VMEM((2, 16, 128), F32),
            pltpu.VMEM((16, 256), BF),
            pltpu.SemaphoreType.DMA((6,)),
        ],
        flops=10**7,
        in_specs=[HBM_SPEC] * 6,
        out_specs=VMEM_SPEC,
    )(condition.reshape(16, 128), ctx_cond.reshape(16, 128), w_shift, w_scale, w_gate, context)
    got = exchange(part, "z")
    lat_parts = along_x(latent)
    w_pair = lax.ppermute(w_out, "c", SWAP)
    summed, ctx_own = call(
        relay_body, (shape((32, 8, 256), F32), shape((256, 256), BF)), flops=10**7
    )(got)
    mod = exchange(summed, ("y", "x", "c"))
    ctx_parts = along_x(ctx_own)
    lat_mine = call(gather_x_body, shape((4, 32, D), BF), flops=10**8)(*lat_parts)
    lat_theirs = lax.ppermute(lat_mine, "c", SWAP)
    ctx_mine = call(gather_x_body, shape((4, 256, 256), BF), flops=10**8)(*ctx_parts)
    ctx_theirs = lax.ppermute(ctx_mine, "c", SWAP)
    ctx_kv = call(
        ctx_kv_body, shape((4, 2, 256, 256), BF), [pltpu.VMEM((256, D), BF)], flops=10**9
    )(ctx_mine, ctx_theirs, mod, gain, w_key, w_value)
    ctx_all = exchange(ctx_kv, "y")

    q, head, tail, gate = call(
        qkv_body,
        (
            shape((256, 256), BF),
            shape((2, 128, 256), BF),
            shape((2, 128, 256), BF),
            shape((1, D), F32),
        ),
        [pltpu.VMEM((256, D), BF)],
        flops=10**9,
    )(lat_mine, lat_theirs, mod, gain, w_query, w_key, w_value)
    count = 64
    prev = lax.ppermute(tail, SP, [(i, i + 1) for i in range(count - 1)])
    nxt = lax.ppermute(head, SP, [(i + 1, i) for i in range(count - 1)])
    table = jnp.pad(rel_bias, ((0, 0), (0, 1), (0, 97)))
    bias = call(
        functools.partial(bias_body, 512),
        shape((2, 2, 3, 128, 128), F32),
        [pltpu.VMEM((15, 4, 32, 128), F32)],
        flops=10**8,
    )(table)
    att, away = call(
        attend_body, (shape((128, 256), BF), shape((128, 256), BF)), flops=10**9
    )(q, prev, head, tail, nxt, bias, ctx_all)
    other = lax.ppermute(away, "c", SWAP)
    parts = call(out_proj_body, shape((4, 32, D), BF), flops=10**9)(att, other, w_out, w_pair)
    arrived = exchange(parts, "x")
    return call(final_body, shape((32, D), BF))(arrived, latent, gate)


def solution(mesh):
    torus = Mesh(mesh.devices.reshape(16, 4, 4, 2), ALL)
    return jax.shard_map(
        on_device,
        mesh=torus,
        in_specs=(
            P(ALL, None),
            P(SP, None),
            P(),
            P(),
            P(),
            P(SP, TP),
            P(SP, TP),
            P(SP, TP),
            P(None, TP),
            P(None, TP),
            P(None, TP),
            P(TP, None),
            P(),
        ),
        out_specs=P(ALL, None),
        check_vma=False,
    )
```

```python
import functools

import jax
import jax.numpy as jnp
from jax import lax
from jax.experimental import pallas as pl
from jax.experimental.pallas import tpu as pltpu
from jax.sharding import Mesh
from jax.sharding import PartitionSpec as P


HEAD_DIM = 128
GRID_W = 32
WIN_H = 8
WIN_W = 16
D = 2048
SP = ("z", "y")
TP = ("x", "c")
ALL = ("z", "y", "x", "c")
NORM_EPS = 1e-06
NEG_BIG = -1e30
LOG2E = 1.4426950408889634
BF = jnp.bfloat16
F32 = jnp.float32


VMEM_SPEC = pl.BlockSpec(memory_space=pltpu.VMEM)
HBM_SPEC = pl.BlockSpec(memory_space=pltpu.HBM)


def call(body, outs, scratch=(), flops=0, vmem=8 << 20, **specs):
    return pl.pallas_call(
        body,
        out_shape=outs,
        **specs,
        scratch_shapes=list(scratch),
        cost_estimate=pl.CostEstimate(flops=flops, bytes_accessed=0, transcendentals=0),
        compiler_params=pltpu.CompilerParams(vmem_limit_bytes=vmem),
    )


def in_hbm(array):
    return pltpu.with_memory_space_constraint(array, pltpu.HBM)


def shape(dims, dtype):
    return jax.ShapeDtypeStruct(dims, dtype)


def pack_rows(rows):
    high = [row.astype(BF).astype(F32) for row in rows]
    low = [rows[i] - high[i] for i in (0, 2, 4)]
    return jnp.concatenate(high + low, axis=0).astype(BF)


def unpack_rows(total):
    rows = [total[i : i + 1, :] for i in range(8)]
    return [rows[0] + rows[5], rows[1], rows[2] + rows[6], rows[3], rows[4] + rows[7]]


def mod_partial_body(
    cond_hbm, ctxc_hbm, wsh_hbm, wsc_hbm, wg_hbm, ctx_hbm, out_ref, pad_ref, act_ref, ctx_ref, sems
):
    sp = lax.axis_index("z") * 4 + lax.axis_index("y")
    tp = lax.axis_index("x") * 2 + lax.axis_index("c")
    row = sp // 4
    off = pl.multiple_of((sp % 4) * 32, 32)
    zero = jnp.zeros((32, 768), BF)
    for i in range(4):
        pad_ref[i * 32 : (i + 1) * 32] = zero
    cols = pl.ds(pl.multiple_of(tp * 256, 256), 256)
    copies = [
        pltpu.make_async_copy(src, dst, sems.at[i])
        for i, (src, dst) in enumerate(
            (
                (cond_hbm, act_ref.at[0]),
                (ctxc_hbm, act_ref.at[1]),
                (wsh_hbm, pad_ref.at[pl.ds(off, 32), 0:256]),
                (wsc_hbm, pad_ref.at[pl.ds(off, 32), 256:512]),
                (wg_hbm, pad_ref.at[pl.ds(off, 32), 512:768]),
                (ctx_hbm.at[:, cols], ctx_ref),
            )
        )
    ]
    for copy in copies:
        copy.start()
    for copy in copies:
        copy.wait()
    cond = act_ref[0, pl.ds(row, 1), :]
    ctxc = act_ref[1, pl.ds(row, 1), :]
    act = jnp.concatenate([cond, ctxc] * 4, axis=0)
    act = (act / (1.0 + jnp.exp(-act))).astype(BF)
    res = jnp.dot(act, pad_ref[...], preferred_element_type=F32)
    packed = pack_rows(
        [res[0:1, 0:256], res[1:2, 0:256], res[0:1, 256:512], res[1:2, 256:512], res[0:1, 512:768]]
    )
    ctx = ctx_ref[...]
    for i in range(out_ref.shape[0]):
        out_ref[i, 0:16] = ctx
        out_ref[i, 16:24] = packed


def relay_body(in_ref, out_ref):
    total = pack_rows(unpack_rows(jnp.sum(in_ref[:, 16:24, :].astype(F32), axis=0)))
    ctx = in_ref[:, 0:16, :].reshape(256, 256)
    for i in range(out_ref.shape[0]):
        out_ref[i, 0:256] = ctx
        out_ref[i, 256:264] = total


def relay_mod_body(in_ref, out_ref):
    total = jnp.concatenate([in_ref[x, 256:264, :] for x in range(4)], axis=1)
    for i in range(out_ref.shape[0]):
        out_ref[i] = total


def mod_row(mod_ref, x, c, kind):
    cols = slice(x * 256, (x + 1) * 256)
    total = mod_ref[c, :, cols].astype(F32)
    for y in range(1, 4):
        total = total + mod_ref[y * 2 + c, :, cols].astype(F32)
    return unpack_rows(total)[kind]


def gather_x_body(own_ref, p1_ref, p2_ref, p3_ref, out_ref):
    x = lax.axis_index("x")
    for d, ref in enumerate((own_ref, p1_ref, p2_ref, p3_ref)):
        out_ref[lax.rem(x - d + 4, 4)] = ref[...]


def ctx_kv_body(mine_ref, theirs_ref, mod_ref, gain_ref, wk_ref, wv_ref, out_ref, xn_ref):
    core = lax.axis_index("c")
    square = jnp.zeros((256, 256), F32)
    for ref in (mine_ref, theirs_ref):
        for j in range(4):
            x = ref[j, 0:256].astype(F32)
            square = square + x * x
    inv = lax.rsqrt(jnp.sum(square, axis=-1, keepdims=True) * (1.0 / D) + NORM_EPS)
    for ref, c in ((mine_ref, core), (theirs_ref, 1 - core)):
        total = mod_ref[c].astype(F32)
        for y in range(1, 4):
            total = total + mod_ref[y * 2 + c].astype(F32)
        for j in range(4):
            cols = pl.ds(pl.multiple_of((2 * j + c) * 256, 256), 256)
            part = total[:, j * 256 : (j + 1) * 256]
            gain = gain_ref[:, cols] * (1.0 + part[3:4])
            x = ref[j, 0:256].astype(F32)
            xn_ref[:, cols] = (x * inv * gain + part[1:2]).astype(BF)
    xn = xn_ref[...]
    k = jnp.dot(xn, wk_ref[...], preferred_element_type=F32).astype(BF)
    for i in range(out_ref.shape[0]):
        out_ref[i, 0] = k
    v = jnp.dot(xn, wv_ref[...], preferred_element_type=F32).astype(BF)
    for i in range(out_ref.shape[0]):
        out_ref[i, 1] = v


def table_body(in_ref, out_ref):
    out_ref[...] = jnp.zeros_like(out_ref)
    out_ref[:, 0:15, 0:31] = in_ref[...]


def qkv_body(
    mine_ref, theirs_ref, mod_ref, gain_ref, wq_hbm, wk_ref, wv_ref,
    q_ref, head_ref, tail_ref, gate_ref, xn_ref, wq_ref, sem,
):
    copy = pltpu.make_async_copy(wq_hbm, wq_ref, sem)
    copy.start()
    core = lax.axis_index("c")
    mods = [[mod_row(mod_ref, i // 2, i % 2, kind) for i in range(8)] for kind in (0, 2, 4)]
    shift, scale, gate = (jnp.concatenate(rows, axis=1) for rows in mods)
    gain = gain_ref[...] * (1.0 + scale)
    gate_ref[...] = gate
    for ref, c in ((mine_ref, core), (theirs_ref, 1 - core)):
        for j in range(4):
            x = ref[j].astype(F32)
            inv = lax.rsqrt(jnp.sum(x * x, axis=-1, keepdims=True) * (1.0 / D) + NORM_EPS)
            rows = pl.ds(pl.multiple_of((2 * j + c) * 32, 32), 32)
            xn_ref[rows, :] = (x * inv * gain + shift).astype(BF)
    xn = xn_ref[...]
    for i, w_ref in enumerate((wk_ref, wv_ref)):
        res = jnp.dot(xn, w_ref[...], preferred_element_type=F32).astype(BF)
        head_ref[i] = res[:128]
        tail_ref[i] = res[128:]
    copy.wait()
    q = jnp.dot(xn_ref[...], wq_ref[...], preferred_element_type=F32)
    q_ref[...] = (q * (LOG2E * HEAD_DIM**-0.5)).astype(BF)


def bias_body(rows_total, tab_ref, out_ref, exp_ref):
    sp = lax.axis_index("z") * 4 + lax.axis_index("y")
    tp = lax.axis_index("x") * 2 + lax.axis_index("c")
    first = sp * 8
    lane = lax.broadcasted_iota(jnp.int32, (32, 128), 1)
    col = lax.broadcasted_iota(jnp.int32, (32, 128), 0)
    key_col = lane % 32
    start = jnp.clip(col - WIN_W // 2, 0, GRID_W - WIN_W)
    col_in = (key_col >= start) & (key_col < start + WIN_W)
    quarter = lane // 32
    for h in range(2):
        tab = tab_ref[tp * 2 + h] * LOG2E
        for d in range(15):
            line = jnp.broadcast_to(tab[d : d + 1, :], (32, 128))
            for p in range(4):
                exp_ref[d, p] = pltpu.roll(line, (32 * p - 15) % 128, 1, stride=1, stride_axis=0)
        for r in range(8):
            a = jnp.clip(first + r - WIN_H // 2, 0, rows_total - WIN_H) - first + WIN_H // 2
            half = r // 4
            for s in range(3):
                seg = half + s
                block = jnp.full((32, 128), NEG_BIG, F32)
                for p in range(4):
                    k = seg * 4 + p
                    d = k - r + 3
                    if 0 <= d < 15:
                        ok = (k >= a) & (k < a + WIN_H)
                        block = jnp.where(
                            (quarter == p) & col_in & ok, exp_ref[d, p], block
                        )
                out_ref[h, half, s, (r % 4) * 32 : (r % 4) * 32 + 32, :] = block


def attend_body(
    q_hbm, prev_ref, head_hbm, tail_hbm, next_ref, bias_hbm, ctx_ref,
    mine_ref, other_ref, q_ref, kv_ref, bias_ref, sems,
):
    copies = [
        pltpu.make_async_copy(src, dst, sems.at[i])
        for i, (src, dst) in enumerate(
            (
                (q_hbm, q_ref),
                (head_hbm, kv_ref.at[0]),
                (tail_hbm, kv_ref.at[1]),
                (bias_hbm, bias_ref),
            )
        )
    ]
    for copy in copies:
        copy.start()
    segs = (prev_ref, kv_ref.at[0], kv_ref.at[1], next_ref)
    core = lax.axis_index("c")
    nt = (((1,), (1,)), ((), ()))
    copies[0].wait()
    for h in range(2):
        hc = slice(h * 128, (h + 1) * 128)
        kc = ctx_ref[:, 0, :, hc].reshape(1024, 128)
        vc = ctx_ref[:, 1, :, hc].reshape(1024, 128)
        s_ctx = lax.dot_general(q_ref[:, hc], kc, nt, preferred_element_type=F32)
        if h == 0:
            for copy in copies[1:]:
                copy.wait()
        s_win = [
            [
                lax.dot_general(
                    q_ref[half * 128 : (half + 1) * 128, hc],
                    segs[half + s][0, :, hc],
                    nt,
                    preferred_element_type=F32,
                )
                + bias_ref[h, half, s]
                for half in range(2)
            ]
            for s in range(3)
        ]
        s_win = [jnp.concatenate(pair, axis=0) for pair in s_win]
        peak = jnp.maximum(jnp.maximum(s_win[0], s_win[1]), s_win[2])
        for i in range(8):
            peak = jnp.maximum(peak, s_ctx[:, i * 128 : (i + 1) * 128])
        top = jnp.max(peak, axis=-1, keepdims=True)
        e_ctx = jnp.exp2(s_ctx - top)
        e_win = [jnp.exp2(s - top) for s in s_win]
        part = e_win[0] + e_win[1] + e_win[2]
        for i in range(8):
            part = part + e_ctx[:, i * 128 : (i + 1) * 128]
        total = jnp.sum(part, axis=-1, keepdims=True)
        acc = jnp.dot(e_ctx.astype(BF), vc, preferred_element_type=F32)
        for half in range(2):
            rows = slice(half * 128, (half + 1) * 128)
            acc_half = acc[rows]
            for s in range(3):
                acc_half = acc_half + jnp.dot(
                    e_win[s][rows].astype(BF),
                    segs[half + s][1, :, hc],
                    preferred_element_type=F32,
                )
            out = (acc_half / total[rows]).astype(BF)
            for i in range(2):
                even = out[i * 64 : i * 64 + 32]
                odd = out[i * 64 + 32 : i * 64 + 64]
                rows = slice((half * 2 + i) * 32, (half * 2 + i + 1) * 32)
                mine_ref[rows, hc] = jnp.where(core == 0, even, odd)
                other_ref[rows, hc] = jnp.where(core == 0, odd, even)


def out_own_body(mine_ref, w_ref, out_ref):
    out_ref[...] = jnp.dot(mine_ref[...], w_ref[...], preferred_element_type=F32)


def out_proj_body(own_ref, got_ref, wp_ref, out_ref):
    res = own_ref[...] + jnp.dot(got_ref[...], wp_ref[...], preferred_element_type=F32)
    out_ref[...] = res.astype(BF).reshape(4, 32, D)


def final_body(parts_ref, lat_ref, gate_ref, out_ref):
    branch = jnp.sum(parts_ref[...].astype(F32), axis=0)
    out_ref[...] = (lat_ref[...].astype(F32) + gate_ref[...] * branch).astype(BF)


def exchange(blocks, axes):
    return lax.all_to_all(blocks, axes, 0, 0, tiled=True)


SWAP = [(0, 1), (1, 0)]


def along_x(own):
    parts = [own]
    for d in (1, 2, 3):
        parts.append(lax.ppermute(own, "x", [(i, (i + d) % 4) for i in range(4)]))
    return parts


def on_device(
    latent,
    context,
    condition,
    ctx_cond,
    norm_gain,
    w_shift,
    w_scale,
    w_gate,
    w_query,
    w_key,
    w_value,
    w_out,
    rel_bias,
):
    gain = norm_gain.reshape(1, D)
    part = call(
        mod_partial_body,
        shape((16, 24, 256), BF),
        [
            pltpu.VMEM((128, 768), BF),
            pltpu.VMEM((2, 16, 128), F32),
            pltpu.VMEM((16, 256), BF),
            pltpu.SemaphoreType.DMA((6,)),
        ],
        flops=10**7,
        in_specs=[HBM_SPEC] * 6,
        out_specs=VMEM_SPEC,
    )(*map(in_hbm, (condition.reshape(16, 128), ctx_cond.reshape(16, 128), w_shift, w_scale, w_gate, context)))
    got = exchange(part, "z")
    lat_parts = along_x(latent)
    table = call(table_body, shape((16, 16, 128), F32), flops=10**7)(rel_bias)
    w_pair = lax.ppermute(w_out, "c", SWAP)
    relayed = call(relay_body, shape((4, 264, 256), BF), flops=10**7)(got)
    ctx_mine = exchange(relayed, "x")
    lat_mine = call(gather_x_body, shape((4, 32, D), BF), flops=10**8)(*lat_parts)
    lat_theirs = lax.ppermute(lat_mine, "c", SWAP)
    mod_own = call(relay_mod_body, shape((8, 8, 1024), BF), flops=10**7)(ctx_mine)
    mod = exchange(mod_own, ("y", "c"))
    ctx_theirs = lax.ppermute(ctx_mine, "c", SWAP)
    ctx_kv = call(
        ctx_kv_body, shape((4, 2, 256, 256), BF), [pltpu.VMEM((256, D), BF)], flops=10**9
    )(ctx_mine, ctx_theirs, mod, gain, w_key, w_value)
    ctx_all = exchange(ctx_kv, "y")

    q, head, tail, gate = call(
        qkv_body,
        (
            shape((256, 256), BF),
            shape((2, 128, 256), BF),
            shape((2, 128, 256), BF),
            shape((1, D), F32),
        ),
        [pltpu.VMEM((256, D), BF), pltpu.VMEM((D, 256), BF), pltpu.SemaphoreType.DMA],
        flops=2 * 10**9,
        in_specs=[VMEM_SPEC] * 4 + [HBM_SPEC] + [VMEM_SPEC] * 2,
        out_specs=[VMEM_SPEC] * 4,
        vmem=16 << 20,
    )(lat_mine, lat_theirs, mod, gain, in_hbm(w_query), w_key, w_value)
    prev = lax.ppermute(tail, SP, [(i, i + 1) for i in range(63)])
    nxt = lax.ppermute(head, SP, [(i + 1, i) for i in range(63)])
    bias = call(
        functools.partial(bias_body, 512),
        shape((2, 2, 3, 128, 128), F32),
        [pltpu.VMEM((15, 4, 32, 128), F32)],
        flops=10**8,
    )(table)
    att, away = call(
        attend_body,
        (shape((128, 256), BF), shape((128, 256), BF)),
        [
            pltpu.VMEM((256, 256), BF),
            pltpu.VMEM((2, 2, 128, 256), BF),
            pltpu.VMEM((2, 2, 3, 128, 128), F32),
            pltpu.SemaphoreType.DMA((4,)),
        ],
        flops=10**9,
        in_specs=[HBM_SPEC, VMEM_SPEC, HBM_SPEC, HBM_SPEC, VMEM_SPEC, HBM_SPEC, VMEM_SPEC],
        out_specs=[VMEM_SPEC] * 2,
    )(in_hbm(q), prev, in_hbm(head), in_hbm(tail), nxt, in_hbm(bias), ctx_all)
    other = lax.ppermute(away, "c", SWAP)
    own = call(out_own_body, shape((128, D), F32), flops=10**9)(att, w_out)
    parts = call(out_proj_body, shape((4, 32, D), BF), flops=10**9)(own, other, w_pair)
    arrived = exchange(parts, "x")
    return call(final_body, shape((32, D), BF))(arrived, latent, gate)


def solution(mesh):
    torus = Mesh(mesh.devices.reshape(16, 4, 4, 2), ALL)
    return jax.shard_map(
        on_device,
        mesh=torus,
        in_specs=(
            P(ALL, None),
            P(SP, None),
            P(),
            P(),
            P(),
            P(SP, TP),
            P(SP, TP),
            P(SP, TP),
            P(None, TP),
            P(None, TP),
            P(None, TP),
            P(TP, None),
            P(),
        ),
        out_specs=P(ALL, None),
        check_vma=False,
    )
```

```python
import functools

import jax
import jax.numpy as jnp
from jax import lax
from jax.experimental import pallas as pl
from jax.experimental.pallas import tpu as pltpu
from jax.sharding import Mesh
from jax.sharding import PartitionSpec as P


HEAD_DIM = 128
GRID_W = 32
WIN_H = 8
WIN_W = 16
D = 2048
Z = ("zh", "zl")
SP = ("zh", "zl", "y")
TP = ("x", "c")
ALL = ("zh", "zl", "y", "x", "c")
NORM_EPS = 1e-06
NEG_BIG = -1e30
LOG2E = 1.4426950408889634
BF = jnp.bfloat16
F32 = jnp.float32


VMEM_SPEC = pl.BlockSpec(memory_space=pltpu.VMEM)
HBM_SPEC = pl.BlockSpec(memory_space=pltpu.HBM)


def call(body, outs, scratch=(), flops=0, vmem=8 << 20, **specs):
    return pl.pallas_call(
        body,
        out_shape=outs,
        **specs,
        scratch_shapes=list(scratch),
        cost_estimate=pl.CostEstimate(flops=flops, bytes_accessed=0, transcendentals=0),
        compiler_params=pltpu.CompilerParams(vmem_limit_bytes=vmem),
    )


def in_hbm(array):
    return pltpu.with_memory_space_constraint(array, pltpu.HBM)


def shape(dims, dtype):
    return jax.ShapeDtypeStruct(dims, dtype)


def pack_rows(rows):
    high = [row.astype(BF).astype(F32) for row in rows]
    low = [rows[i] - high[i] for i in (0, 2, 4)]
    return jnp.concatenate(high + low, axis=0)


def unpack_rows(total):
    rows = [total[i : i + 1, :] for i in range(8)]
    return [rows[0] + rows[5], rows[1], rows[2] + rows[6], rows[3], rows[4] + rows[7]]


def mod_partial_body(
    cond_hbm, ctxc_hbm, wsh_hbm, wsc_hbm, wg_hbm, ctx_hbm, out_ref, pad_ref, act_ref, ctx_ref, sems
):
    sp = lax.axis_index(SP)
    tp = lax.axis_index("x") * 2 + lax.axis_index("c")
    row = sp // 4
    off = pl.multiple_of((sp % 4) * 32, 32)
    zero = jnp.zeros((32, 768), BF)
    for i in range(4):
        pad_ref[i * 32 : (i + 1) * 32] = zero
    cols = pl.ds(pl.multiple_of(tp * 256, 256), 256)
    copies = [
        pltpu.make_async_copy(src, dst, sems.at[i])
        for i, (src, dst) in enumerate(
            (
                (cond_hbm, act_ref.at[0]),
                (ctxc_hbm, act_ref.at[1]),
                (wsh_hbm, pad_ref.at[pl.ds(off, 32), 0:256]),
                (wsc_hbm, pad_ref.at[pl.ds(off, 32), 256:512]),
                (wg_hbm, pad_ref.at[pl.ds(off, 32), 512:768]),
                (ctx_hbm.at[:, cols], ctx_ref),
            )
        )
    ]
    for copy in copies:
        copy.start()
    for copy in copies:
        copy.wait()
    cond = act_ref[0, pl.ds(row, 1), :]
    ctxc = act_ref[1, pl.ds(row, 1), :]
    act = jnp.concatenate([cond, ctxc] * 4, axis=0)
    act = (act / (1.0 + jnp.exp(-act))).astype(BF)
    res = jnp.dot(act, pad_ref[...], preferred_element_type=F32)
    packed = pack_rows(
        [res[0:1, 0:256], res[1:2, 0:256], res[0:1, 256:512], res[1:2, 256:512], res[0:1, 512:768]]
    )
    ctx = ctx_ref[...].astype(F32)
    blocks = [jnp.concatenate([ctx[i * 8 : i * 8 + 8], packed], axis=0).astype(BF) for i in range(2)]
    for i in range(out_ref.shape[0]):
        out_ref[i] = blocks[i % 2]


def relay_body(in_ref, out_ref):
    got = in_ref[...].astype(F32)
    total = pack_rows(unpack_rows(jnp.sum(got[:, 8:16, :], axis=0)))
    block = jnp.concatenate([got[:, 0:8, :].reshape(128, 256), total], axis=0).astype(BF)
    for i in range(out_ref.shape[0]):
        out_ref[i] = block


def column_block(x, c):
    return pl.ds(pl.multiple_of((2 * x + c) * 256, 256), 256)


def relay_mod_body(mine_ref, theirs_ref, out_ref):
    core = lax.axis_index("c")
    for ref, c in ((mine_ref, core), (theirs_ref, 1 - core)):
        for x in range(4):
            block = ref[x, 128:136, :]
            for i in range(out_ref.shape[0]):
                out_ref[i, :, column_block(x, c)] = block


def sum_over_y(mod_ref, cols):
    total = mod_ref[0, :, cols].astype(F32)
    for y in range(1, 4):
        total = total + mod_ref[y, :, cols].astype(F32)
    return total


def gather_x_body(own_ref, p1_ref, p2_ref, p3_ref, out_ref):
    x = lax.axis_index("x")
    for d, ref in enumerate((own_ref, p1_ref, p2_ref, p3_ref)):
        out_ref[lax.rem(x - d + 4, 4)] = ref[...]


def ctx_kv_body(mine_ref, theirs_ref, mod_ref, gain_hbm, wk_ref, wv_ref, out_ref, xn_ref, gain_ref, sem):
    copy = pltpu.make_async_copy(gain_hbm, gain_ref, sem)
    copy.start()
    core = lax.axis_index("c")
    square = jnp.zeros((128, 256), F32)
    for ref in (mine_ref, theirs_ref):
        for j in range(4):
            x = ref[j, 0:128].astype(F32)
            square = square + x * x
    inv = lax.rsqrt(jnp.sum(square, axis=-1, keepdims=True) * (1.0 / D) + NORM_EPS)
    copy.wait()
    for ref, c in ((mine_ref, core), (theirs_ref, 1 - core)):
        for j in range(4):
            cols = column_block(j, c)
            part = sum_over_y(mod_ref, cols)
            gain = gain_ref[:, cols] * (1.0 + part[3:4])
            x = ref[j, 0:128].astype(F32)
            xn_ref[:, cols] = (x * inv * gain + part[1:2]).astype(BF)
    xn = xn_ref[...]
    k = jnp.dot(xn, wk_ref[...], preferred_element_type=F32).astype(BF)
    for i in range(out_ref.shape[0]):
        out_ref[i, 0] = k
    v = jnp.dot(xn, wv_ref[...], preferred_element_type=F32).astype(BF)
    for i in range(out_ref.shape[0]):
        out_ref[i, 1] = v


def table_body(in_ref, out_ref):
    out_ref[...] = jnp.zeros_like(out_ref)
    out_ref[:, 0:15, 0:31] = in_ref[...]


def kv_body(
    mine_hbm, theirs_hbm, mod_ref, gain_hbm, wk_ref, wv_ref,
    head_ref, tail_ref, gate_ref, xn_ref, lat_ref, gain_ref, sems,
):
    copies = [
        pltpu.make_async_copy(src, lat_ref.at[i], sems.at[i])
        for i, src in enumerate((mine_hbm, theirs_hbm))
    ] + [pltpu.make_async_copy(gain_hbm, gain_ref, sems.at[2])]
    for copy in copies:
        copy.start()
    core = lax.axis_index("c")
    shift, _, scale, _, gate = unpack_rows(sum_over_y(mod_ref, slice(None)))
    gate_ref[...] = gate
    copies[2].wait()
    gain = gain_ref[...] * (1.0 + scale)
    for i, c in enumerate((core, 1 - core)):
        copies[i].wait()
        for j in range(4):
            x = lat_ref[i, j].astype(F32)
            inv = lax.rsqrt(jnp.sum(x * x, axis=-1, keepdims=True) * (1.0 / D) + NORM_EPS)
            rows = pl.ds(pl.multiple_of((2 * j + c) * 32, 32), 32)
            xn_ref[rows, :] = (x * inv * gain + shift).astype(BF)
    xn = xn_ref[...]
    for i, w_ref in enumerate((wk_ref, wv_ref)):
        res = jnp.dot(xn, w_ref[...], preferred_element_type=F32).astype(BF)
        head_ref[i] = res[:128]
        tail_ref[i] = res[128:]


def query_body(xn_ref, wq_ref, q_ref):
    q = jnp.dot(xn_ref[...], wq_ref[...], preferred_element_type=F32)
    q_ref[...] = (q * (LOG2E * HEAD_DIM**-0.5)).astype(BF)


def bias_body(rows_total, tab_ref, out_ref, exp_ref):
    sp = lax.axis_index(SP)
    tp = lax.axis_index("x") * 2 + lax.axis_index("c")
    first = sp * 8
    lane = lax.broadcasted_iota(jnp.int32, (32, 128), 1)
    col = lax.broadcasted_iota(jnp.int32, (32, 128), 0)
    key_col = lane % 32
    start = jnp.clip(col - WIN_W // 2, 0, GRID_W - WIN_W)
    col_in = (key_col >= start) & (key_col < start + WIN_W)
    quarter = lane // 32
    for h in range(2):
        tab = tab_ref[tp * 2 + h] * LOG2E
        for d in range(15):
            line = jnp.broadcast_to(tab[d : d + 1, :], (32, 128))
            for p in range(4):
                exp_ref[d, p] = pltpu.roll(line, (32 * p - 15) % 128, 1, stride=1, stride_axis=0)
        for r in range(8):
            a = jnp.clip(first + r - WIN_H // 2, 0, rows_total - WIN_H) - first + WIN_H // 2
            half = r // 4
            for s in range(3):
                seg = half + s
                block = jnp.full((32, 128), NEG_BIG, F32)
                for p in range(4):
                    k = seg * 4 + p
                    d = k - r + 3
                    if 0 <= d < 15:
                        ok = (k >= a) & (k < a + WIN_H)
                        block = jnp.where(
                            (quarter == p) & col_in & ok, exp_ref[d, p], block
                        )
                out_ref[h, half, s, (r % 4) * 32 : (r % 4) * 32 + 32, :] = block


def attend_body(
    q_hbm, prev_ref, head_hbm, tail_hbm, next_ref, bias_hbm, ctx_ref, w_hbm, wp_hbm,
    mine_ref, other_ref, w_ref, q_ref, kv_ref, bias_ref, sems,
):
    copies = [
        pltpu.make_async_copy(src, dst, sems.at[i])
        for i, (src, dst) in enumerate(
            (
                (q_hbm, q_ref),
                (head_hbm, kv_ref.at[0]),
                (tail_hbm, kv_ref.at[1]),
                (bias_hbm, bias_ref),
                (w_hbm, w_ref.at[0]),
                (wp_hbm, w_ref.at[1]),
            )
        )
    ]
    for copy in copies:
        copy.start()
    segs = (prev_ref, kv_ref.at[0], kv_ref.at[1], next_ref)
    core = lax.axis_index("c")
    nt = (((1,), (1,)), ((), ()))
    copies[0].wait()
    for h in range(2):
        hc = slice(h * 128, (h + 1) * 128)
        kc = ctx_ref[:, 0, :, hc].reshape(1024, 128)
        vc = ctx_ref[:, 1, :, hc].reshape(1024, 128)
        s_ctx = lax.dot_general(q_ref[:, hc], kc, nt, preferred_element_type=F32)
        if h == 0:
            for copy in copies[1:4]:
                copy.wait()
        s_win = [
            [
                lax.dot_general(
                    q_ref[half * 128 : (half + 1) * 128, hc],
                    segs[half + s][0, :, hc],
                    nt,
                    preferred_element_type=F32,
                )
                + bias_ref[h, half, s]
                for half in range(2)
            ]
            for s in range(3)
        ]
        s_win = [jnp.concatenate(pair, axis=0) for pair in s_win]
        peak = jnp.maximum(jnp.maximum(s_win[0], s_win[1]), s_win[2])
        for i in range(8):
            peak = jnp.maximum(peak, s_ctx[:, i * 128 : (i + 1) * 128])
        top = jnp.max(peak, axis=-1, keepdims=True)
        e_ctx = jnp.exp2(s_ctx - top)
        e_win = [jnp.exp2(s - top) for s in s_win]
        part = e_win[0] + e_win[1] + e_win[2]
        for i in range(8):
            part = part + e_ctx[:, i * 128 : (i + 1) * 128]
        total = jnp.sum(part, axis=-1, keepdims=True)
        acc = jnp.dot(e_ctx.astype(BF), vc, preferred_element_type=F32)
        for half in range(2):
            rows = slice(half * 128, (half + 1) * 128)
            acc_half = acc[rows]
            for s in range(3):
                acc_half = acc_half + jnp.dot(
                    e_win[s][rows].astype(BF),
                    segs[half + s][1, :, hc],
                    preferred_element_type=F32,
                )
            out = (acc_half / total[rows]).astype(BF)
            for i in range(2):
                even = out[i * 64 : i * 64 + 32]
                odd = out[i * 64 + 32 : i * 64 + 64]
                rows = slice((half * 2 + i) * 32, (half * 2 + i + 1) * 32)
                mine_ref[rows, hc] = jnp.where(core == 0, even, odd)
                other_ref[rows, hc] = jnp.where(core == 0, odd, even)
    for copy in copies[4:]:
        copy.wait()


def out_own_body(mine_ref, w_ref, out_ref):
    out_ref[...] = jnp.dot(mine_ref[...], w_ref[0], preferred_element_type=F32)


def out_proj_body(own_ref, got_ref, w_ref, out_ref):
    res = own_ref[...] + jnp.dot(got_ref[...], w_ref[1], preferred_element_type=F32)
    out_ref[...] = res.astype(BF).reshape(4, 32, D)


def final_body(parts_ref, lat_ref, gate_ref, out_ref):
    branch = jnp.sum(parts_ref[...].astype(F32), axis=0)
    out_ref[...] = (lat_ref[...].astype(F32) + gate_ref[...] * branch).astype(BF)


def exchange(blocks, axes):
    return lax.all_to_all(blocks, axes, 0, 0, tiled=True)


SWAP = [(0, 1), (1, 0)]


def along_x(own):
    parts = [own]
    for d in (1, 2, 3):
        parts.append(lax.ppermute(own, "x", [(i, (i + d) % 4) for i in range(4)]))
    return parts


def on_device(
    latent,
    context,
    condition,
    ctx_cond,
    norm_gain,
    w_shift,
    w_scale,
    w_gate,
    w_query,
    w_key,
    w_value,
    w_out,
    rel_bias,
):
    gain = in_hbm(norm_gain.reshape(1, D))
    part = call(
        mod_partial_body,
        shape((16, 16, 256), BF),
        [
            pltpu.VMEM((128, 768), BF),
            pltpu.VMEM((2, 16, 128), F32),
            pltpu.VMEM((16, 256), BF),
            pltpu.SemaphoreType.DMA((6,)),
        ],
        flops=10**7,
        in_specs=[HBM_SPEC] * 6,
        out_specs=VMEM_SPEC,
    )(*map(in_hbm, (condition.reshape(16, 128), ctx_cond.reshape(16, 128), w_shift, w_scale, w_gate, context)))
    got = exchange(part, Z)
    lat_parts = along_x(latent)
    table = call(table_body, shape((16, 16, 128), F32), flops=10**7)(rel_bias)
    w_pair = lax.ppermute(w_out, "c", SWAP)
    relayed = call(relay_body, shape((4, 136, 256), BF), flops=10**7)(got)
    ctx_mine = exchange(relayed, "x")
    lat_mine = call(gather_x_body, shape((4, 32, D), BF), flops=10**8)(*lat_parts)
    lat_theirs = lax.ppermute(lat_mine, "c", SWAP)
    ctx_theirs = lax.ppermute(ctx_mine, "c", SWAP)
    mod_own = call(relay_mod_body, shape((4, 8, D), BF), flops=10**7)(ctx_mine, ctx_theirs)
    mod = exchange(mod_own, "y")
    ctx_kv = call(
        ctx_kv_body,
        shape((8, 2, 128, 256), BF),
        [pltpu.VMEM((128, D), BF), pltpu.VMEM((1, D), F32), pltpu.SemaphoreType.DMA],
        flops=10**9,
        in_specs=[VMEM_SPEC] * 3 + [HBM_SPEC] + [VMEM_SPEC] * 2,
        out_specs=VMEM_SPEC,
    )(ctx_mine, ctx_theirs, mod, gain, w_key, w_value)
    ctx_all = exchange(ctx_kv, ("zl", "y"))

    head, tail, gate, xn = call(
        kv_body,
        (
            shape((2, 128, 256), BF),
            shape((2, 128, 256), BF),
            shape((1, D), F32),
            shape((256, D), BF),
        ),
        [pltpu.VMEM((2, 4, 32, D), BF), pltpu.VMEM((1, D), F32), pltpu.SemaphoreType.DMA((3,))],
        flops=2 * 10**9,
        in_specs=[HBM_SPEC] * 2 + [VMEM_SPEC, HBM_SPEC] + [VMEM_SPEC] * 2,
        out_specs=[VMEM_SPEC] * 4,
        vmem=16 << 20,
    )(in_hbm(lat_mine), in_hbm(lat_theirs), mod, gain, w_key, w_value)
    q = call(query_body, shape((256, 256), BF), flops=10**9)(xn, w_query)
    prev = lax.ppermute(tail, SP, [(i, i + 1) for i in range(63)])
    nxt = lax.ppermute(head, SP, [(i + 1, i) for i in range(63)])
    bias = call(
        functools.partial(bias_body, 512),
        shape((2, 2, 3, 128, 128), F32),
        [pltpu.VMEM((15, 4, 32, 128), F32)],
        flops=10**8,
    )(table)
    att, away, w_near = call(
        attend_body,
        (shape((128, 256), BF), shape((128, 256), BF), shape((2, 256, D), BF)),
        [
            pltpu.VMEM((256, 256), BF),
            pltpu.VMEM((2, 2, 128, 256), BF),
            pltpu.VMEM((2, 2, 3, 128, 128), F32),
            pltpu.SemaphoreType.DMA((6,)),
        ],
        flops=10**9,
        in_specs=[HBM_SPEC, VMEM_SPEC, HBM_SPEC, HBM_SPEC, VMEM_SPEC, HBM_SPEC, VMEM_SPEC, HBM_SPEC, HBM_SPEC],
        out_specs=[VMEM_SPEC] * 3,
    )(in_hbm(q), prev, in_hbm(head), in_hbm(tail), nxt, in_hbm(bias), ctx_all, in_hbm(w_out), in_hbm(w_pair))
    other = lax.ppermute(away, "c", SWAP)
    own = call(out_own_body, shape((128, D), F32), flops=10**9)(att, w_near)
    parts = call(out_proj_body, shape((4, 32, D), BF), flops=10**9)(own, other, w_near)
    arrived = exchange(parts, "x")
    return call(final_body, shape((32, D), BF))(arrived, latent, gate)


def solution(mesh):
    torus = Mesh(mesh.devices.reshape(8, 2, 4, 4, 2), ALL)
    return jax.shard_map(
        on_device,
        mesh=torus,
        in_specs=(
            P(ALL, None),
            P(SP, None),
            P(),
            P(),
            P(),
            P(SP, TP),
            P(SP, TP),
            P(SP, TP),
            P(None, TP),
            P(None, TP),
            P(None, TP),
            P(TP, None),
            P(),
        ),
        out_specs=P(ALL, None),
        check_vma=False,
    )
```

```python
import functools

import jax
import jax.numpy as jnp
from jax import lax
from jax.experimental import pallas as pl
from jax.experimental.pallas import tpu as pltpu
from jax.sharding import Mesh
from jax.sharding import PartitionSpec as P


HEAD_DIM = 128
GRID_W = 32
WIN_H = 8
WIN_W = 16
D = 2048
Z = ("zh", "zl")
SP = ("zh", "zl", "y")
TP = ("x", "c")
ALL = ("zh", "zl", "y", "x", "c")
NORM_EPS = 1e-06
NEG_BIG = -1e30
LOG2E = 1.4426950408889634
BF = jnp.bfloat16
F32 = jnp.float32


VMEM_SPEC = pl.BlockSpec(memory_space=pltpu.VMEM)
HBM_SPEC = pl.BlockSpec(memory_space=pltpu.HBM)


def call(body, outs, scratch=(), flops=0, vmem=8 << 20, **specs):
    return pl.pallas_call(
        body,
        out_shape=outs,
        **specs,
        scratch_shapes=list(scratch),
        cost_estimate=pl.CostEstimate(flops=flops, bytes_accessed=0, transcendentals=0),
        compiler_params=pltpu.CompilerParams(vmem_limit_bytes=vmem),
    )


def in_hbm(array):
    return pltpu.with_memory_space_constraint(array, pltpu.HBM)


def shape(dims, dtype):
    return jax.ShapeDtypeStruct(dims, dtype)


def pack_rows(rows):
    high = [row.astype(BF).astype(F32) for row in rows]
    low = [rows[i] - high[i] for i in (0, 2, 4)]
    return jnp.concatenate(high + low, axis=0)


def unpack_rows(total):
    rows = [total[i : i + 1, :] for i in range(8)]
    return [rows[0] + rows[5], rows[1], rows[2] + rows[6], rows[3], rows[4] + rows[7]]


def mod_partial_body(
    cond_hbm, ctxc_hbm, wsh_hbm, wsc_hbm, wg_hbm, ctx_hbm, out_ref, pad_ref, act_ref, ctx_ref, sems
):
    sp = lax.axis_index(SP)
    tp = lax.axis_index("x") * 2 + lax.axis_index("c")
    row = sp // 4
    off = pl.multiple_of((sp % 4) * 32, 32)
    zero = jnp.zeros((32, 768), BF)
    for i in range(4):
        pad_ref[i * 32 : (i + 1) * 32] = zero
    cols = pl.ds(pl.multiple_of(tp * 256, 256), 256)
    copies = [
        pltpu.make_async_copy(src, dst, sems.at[i])
        for i, (src, dst) in enumerate(
            (
                (cond_hbm, act_ref.at[0]),
                (ctxc_hbm, act_ref.at[1]),
                (wsh_hbm, pad_ref.at[pl.ds(off, 32), 0:256]),
                (wsc_hbm, pad_ref.at[pl.ds(off, 32), 256:512]),
                (wg_hbm, pad_ref.at[pl.ds(off, 32), 512:768]),
                (ctx_hbm.at[:, cols], ctx_ref),
            )
        )
    ]
    for copy in copies:
        copy.start()
    for copy in copies:
        copy.wait()
    cond = act_ref[0, pl.ds(row, 1), :]
    ctxc = act_ref[1, pl.ds(row, 1), :]
    act = jnp.concatenate([cond, ctxc] * 4, axis=0)
    act = (act / (1.0 + jnp.exp(-act))).astype(BF)
    res = jnp.dot(act, pad_ref[...], preferred_element_type=F32)
    packed = pack_rows(
        [res[0:1, 0:256], res[1:2, 0:256], res[0:1, 256:512], res[1:2, 256:512], res[0:1, 512:768]]
    )
    ctx = ctx_ref[...].astype(F32)
    blocks = [jnp.concatenate([ctx[i * 8 : i * 8 + 8], packed], axis=0).astype(BF) for i in range(2)]
    for i in range(out_ref.shape[0]):
        out_ref[i] = blocks[i % 2]


def relay_body(in_ref, out_ref):
    got = in_ref[...].astype(F32)
    total = pack_rows(unpack_rows(jnp.sum(got[:, 8:16, :], axis=0)))
    block = jnp.concatenate([got[:, 0:8, :].reshape(128, 256), total], axis=0).astype(BF)
    for i in range(out_ref.shape[0]):
        out_ref[i] = block


def column_block(x, c):
    return pl.ds(pl.multiple_of((2 * x + c) * 256, 256), 256)


def relay_mod_body(mine_ref, theirs_ref, out_ref):
    core = lax.axis_index("c")
    for ref, c in ((mine_ref, core), (theirs_ref, 1 - core)):
        for x in range(4):
            block = ref[x, 128:136, :]
            for i in range(out_ref.shape[0]):
                out_ref[i, :, column_block(x, c)] = block


def sum_over_y(mod_ref, cols):
    total = mod_ref[0, :, cols].astype(F32)
    for y in range(1, 4):
        total = total + mod_ref[y, :, cols].astype(F32)
    return total


def gather_x_body(own_ref, p1_ref, p2_ref, p3_ref, out_ref):
    x = lax.axis_index("x")
    for d, ref in enumerate((own_ref, p1_ref, p2_ref, p3_ref)):
        out_ref[lax.rem(x - d + 4, 4)] = ref[...]


def ctx_pre_body(mine_ref, gain_hbm, gain_ref, square_ref, sem):
    copy = pltpu.make_async_copy(gain_hbm, gain_ref, sem)
    copy.start()
    square = jnp.zeros((128, 256), F32)
    for j in range(4):
        x = mine_ref[j, 0:128].astype(F32)
        square = square + x * x
    square_ref[...] = square
    copy.wait()


def ctx_kv_body(mine_ref, theirs_ref, square_ref, mod_ref, gain_ref, wk_ref, wv_ref, out_ref, xn_ref):
    core = lax.axis_index("c")
    square = square_ref[...]
    for j in range(4):
        x = theirs_ref[j, 0:128].astype(F32)
        square = square + x * x
    inv = lax.rsqrt(jnp.sum(square, axis=-1, keepdims=True) * (1.0 / D) + NORM_EPS)
    for ref, c in ((mine_ref, core), (theirs_ref, 1 - core)):
        for j in range(4):
            cols = column_block(j, c)
            part = sum_over_y(mod_ref, cols)
            gain = gain_ref[:, cols] * (1.0 + part[3:4])
            x = ref[j, 0:128].astype(F32)
            xn_ref[:, cols] = (x * inv * gain + part[1:2]).astype(BF)
    xn = xn_ref[...]
    k = jnp.dot(xn, wk_ref[...], preferred_element_type=F32).astype(BF)
    for i in range(out_ref.shape[0]):
        out_ref[i, 0] = k
    v = jnp.dot(xn, wv_ref[...], preferred_element_type=F32).astype(BF)
    for i in range(out_ref.shape[0]):
        out_ref[i, 1] = v


def table_body(in_ref, out_ref):
    out_ref[...] = jnp.zeros_like(out_ref)
    out_ref[:, 0:15, 0:31] = in_ref[...]


def kv_body(
    mine_hbm, theirs_hbm, mod_ref, gain_hbm, wk_ref, wv_ref,
    head_ref, tail_ref, start_ref, gate_ref, xn_ref, lat_ref, gain_ref, sems,
):
    copies = [
        pltpu.make_async_copy(src, lat_ref.at[i], sems.at[i])
        for i, src in enumerate((mine_hbm, theirs_hbm))
    ] + [pltpu.make_async_copy(gain_hbm, gain_ref, sems.at[2])]
    for copy in copies:
        copy.start()
    core = lax.axis_index("c")
    shift, _, scale, _, gate = unpack_rows(sum_over_y(mod_ref, slice(None)))
    gate_ref[...] = gate
    copies[2].wait()
    gain = gain_ref[...] * (1.0 + scale)
    for i, c in enumerate((core, 1 - core)):
        copies[i].wait()
        for j in range(4):
            x = lat_ref[i, j].astype(F32)
            inv = lax.rsqrt(jnp.sum(x * x, axis=-1, keepdims=True) * (1.0 / D) + NORM_EPS)
            rows = pl.ds(pl.multiple_of((2 * j + c) * 32, 32), 32)
            xn_ref[rows, :] = (x * inv * gain + shift).astype(BF)
    xn = xn_ref[...]
    for i, w_ref in enumerate((wk_ref, wv_ref)):
        res = jnp.dot(xn, w_ref[...], preferred_element_type=F32).astype(BF)
        head_ref[i] = res[:128]
        tail_ref[i] = res[128:]
        start_ref[i] = res[:96]


def query_body(xn_ref, wq_ref, q_ref):
    q = jnp.dot(xn_ref[...], wq_ref[...], preferred_element_type=F32)
    q_ref[...] = (q * (LOG2E * HEAD_DIM**-0.5)).astype(BF)


def bias_body(rows_total, tab_ref, out_ref, exp_ref):
    sp = lax.axis_index(SP)
    tp = lax.axis_index("x") * 2 + lax.axis_index("c")
    first = sp * 8
    lane = lax.broadcasted_iota(jnp.int32, (32, 128), 1)
    col = lax.broadcasted_iota(jnp.int32, (32, 128), 0)
    key_col = lane % 32
    start = jnp.clip(col - WIN_W // 2, 0, GRID_W - WIN_W)
    col_in = (key_col >= start) & (key_col < start + WIN_W)
    quarter = lane // 32
    for h in range(2):
        tab = tab_ref[tp * 2 + h] * LOG2E
        for d in range(15):
            line = jnp.broadcast_to(tab[d : d + 1, :], (32, 128))
            for p in range(4):
                exp_ref[d, p] = pltpu.roll(line, (32 * p - 15) % 128, 1, stride=1, stride_axis=0)
        for r in range(8):
            a = jnp.clip(first + r - WIN_H // 2, 0, rows_total - WIN_H) - first + WIN_H // 2
            half = r // 4
            for s in range(3):
                seg = half + s
                block = jnp.full((32, 128), NEG_BIG, F32)
                for p in range(4):
                    k = seg * 4 + p
                    d = k - r + 3
                    if 0 <= d < 15:
                        ok = (k >= a) & (k < a + WIN_H)
                        block = jnp.where(
                            (quarter == p) & col_in & ok, exp_ref[d, p], block
                        )
                out_ref[h, half, s, (r % 4) * 32 : (r % 4) * 32 + 32, :] = block


def attend_body(
    q_hbm, prev_ref, head_hbm, tail_hbm, next_ref, bias_hbm, ctx_ref, w_hbm,
    mine_ref, other_ref, w_ref, q_ref, kv_ref, bias_ref, sems,
):
    copies = [
        pltpu.make_async_copy(src, dst, sems.at[i])
        for i, (src, dst) in enumerate(
            (
                (q_hbm, q_ref),
                (head_hbm, kv_ref.at[0]),
                (tail_hbm, kv_ref.at[1]),
                (bias_hbm, bias_ref),
                (w_hbm, w_ref),
            )
        )
    ]
    for copy in copies:
        copy.start()

    def seg(index, kind, hc):
        if index == 3:
            return jnp.concatenate([next_ref[kind, :, hc], jnp.zeros((32, 128), BF)], axis=0)
        return (prev_ref, kv_ref.at[0], kv_ref.at[1])[index][kind, :, hc]

    core = lax.axis_index("c")
    nt = (((1,), (1,)), ((), ()))
    copies[0].wait()
    heads = [slice(h * 128, (h + 1) * 128) for h in range(2)]
    scores_ctx = [
        lax.dot_general(
            q_ref[:, hc], ctx_ref[:, 0, :, hc].reshape(1024, 128), nt, preferred_element_type=F32
        )
        for hc in heads
    ]
    for copy in copies[1:4]:
        copy.wait()
    scores_win = [
        [
            jnp.concatenate(
                [
                    lax.dot_general(
                        q_ref[half * 128 : (half + 1) * 128, hc],
                        seg(half + s, 0, hc),
                        nt,
                        preferred_element_type=F32,
                    )
                    + bias_ref[h, half, s]
                    for half in range(2)
                ],
                axis=0,
            )
            for s in range(3)
        ]
        for h, hc in enumerate(heads)
    ]
    for h, hc in enumerate(heads):
        vc = ctx_ref[:, 1, :, hc].reshape(1024, 128)
        s_ctx, s_win = scores_ctx[h], scores_win[h]
        peak = jnp.maximum(jnp.maximum(s_win[0], s_win[1]), s_win[2])
        for i in range(8):
            peak = jnp.maximum(peak, s_ctx[:, i * 128 : (i + 1) * 128])
        top = jnp.max(peak, axis=-1, keepdims=True)
        e_ctx = jnp.exp2(s_ctx - top)
        e_win = [jnp.exp2(s - top) for s in s_win]
        part = e_win[0] + e_win[1] + e_win[2]
        for i in range(8):
            part = part + e_ctx[:, i * 128 : (i + 1) * 128]
        total = jnp.sum(part, axis=-1, keepdims=True)
        acc = jnp.dot(e_ctx.astype(BF), vc, preferred_element_type=F32)
        for half in range(2):
            rows = slice(half * 128, (half + 1) * 128)
            acc_half = acc[rows]
            for s in range(3):
                acc_half = acc_half + jnp.dot(
                    e_win[s][rows].astype(BF),
                    seg(half + s, 1, hc),
                    preferred_element_type=F32,
                )
            out = (acc_half / total[rows]).astype(BF)
            for i in range(2):
                even = out[i * 64 : i * 64 + 32]
                odd = out[i * 64 + 32 : i * 64 + 64]
                rows = slice((half * 2 + i) * 32, (half * 2 + i + 1) * 32)
                mine_ref[rows, hc] = jnp.where(core == 0, even, odd)
                other_ref[rows, hc] = jnp.where(core == 0, odd, even)
    for copy in copies[4:]:
        copy.wait()


def out_own_body(mine_ref, w_ref, out_ref):
    out_ref[...] = jnp.dot(mine_ref[...], w_ref[...], preferred_element_type=F32)


def out_proj_body(own_ref, got_ref, w_ref, out_ref):
    res = own_ref[...] + jnp.dot(got_ref[...], w_ref[...], preferred_element_type=F32)
    out_ref[...] = res.astype(BF).reshape(4, 32, D)


def final_body(parts_ref, lat_ref, gate_ref, out_ref):
    branch = jnp.sum(parts_ref[...].astype(F32), axis=0)
    out_ref[...] = (lat_ref[...].astype(F32) + gate_ref[...] * branch).astype(BF)


def exchange(blocks, axes):
    return lax.all_to_all(blocks, axes, 0, 0, tiled=True)


SWAP = [(0, 1), (1, 0)]


def along_x(own):
    parts = [own]
    for d in (1, 2, 3):
        parts.append(lax.ppermute(own, "x", [(i, (i + d) % 4) for i in range(4)]))
    return parts


def on_device(
    latent,
    context,
    condition,
    ctx_cond,
    norm_gain,
    w_shift,
    w_scale,
    w_gate,
    w_query,
    w_key,
    w_value,
    w_out,
    rel_bias,
):
    gain = in_hbm(norm_gain.reshape(1, D))
    part = call(
        mod_partial_body,
        shape((16, 16, 256), BF),
        [
            pltpu.VMEM((128, 768), BF),
            pltpu.VMEM((2, 16, 128), F32),
            pltpu.VMEM((16, 256), BF),
            pltpu.SemaphoreType.DMA((6,)),
        ],
        flops=10**7,
        in_specs=[HBM_SPEC] * 6,
        out_specs=VMEM_SPEC,
    )(*map(in_hbm, (condition.reshape(16, 128), ctx_cond.reshape(16, 128), w_shift, w_scale, w_gate, context)))
    got = exchange(part, Z)
    lat_parts = along_x(latent)
    table = call(table_body, shape((16, 16, 128), F32), flops=10**7)(rel_bias)
    w_pair = lax.ppermute(w_out, "c", SWAP)
    relayed = call(relay_body, shape((4, 136, 256), BF), flops=10**7)(got)
    ctx_mine = exchange(relayed, "x")
    lat_mine = call(gather_x_body, shape((4, 32, D), BF), flops=10**8)(*lat_parts)
    lat_theirs = lax.ppermute(lat_mine, "c", SWAP)
    ctx_theirs = lax.ppermute(ctx_mine, "c", SWAP)
    gain_near, square = call(
        ctx_pre_body,
        (shape((1, D), F32), shape((128, 256), F32)),
        [pltpu.SemaphoreType.DMA],
        flops=10**8,
        in_specs=[VMEM_SPEC, HBM_SPEC],
        out_specs=[VMEM_SPEC] * 2,
    )(ctx_mine, gain)
    mod_own = call(relay_mod_body, shape((4, 8, D), BF), flops=10**7)(ctx_mine, ctx_theirs)
    mod = exchange(mod_own, "y")
    ctx_kv = call(
        ctx_kv_body, shape((8, 2, 128, 256), BF), [pltpu.VMEM((128, D), BF)], flops=10**9
    )(ctx_mine, ctx_theirs, square, mod, gain_near, w_key, w_value)
    ctx_all = exchange(ctx_kv, ("zl", "y"))

    head, tail, start, gate, xn = call(
        kv_body,
        (
            shape((2, 128, 256), BF),
            shape((2, 128, 256), BF),
            shape((2, 96, 256), BF),
            shape((1, D), F32),
            shape((256, D), BF),
        ),
        [pltpu.VMEM((2, 4, 32, D), BF), pltpu.VMEM((1, D), F32), pltpu.SemaphoreType.DMA((3,))],
        flops=2 * 10**9,
        in_specs=[HBM_SPEC] * 2 + [VMEM_SPEC, HBM_SPEC] + [VMEM_SPEC] * 2,
        out_specs=[VMEM_SPEC] * 5,
        vmem=16 << 20,
    )(in_hbm(lat_mine), in_hbm(lat_theirs), mod, gain, w_key, w_value)
    q = call(query_body, shape((256, 256), BF), flops=10**9)(xn, w_query)
    prev = lax.ppermute(tail, SP, [(i, i + 1) for i in range(63)])
    nxt = lax.ppermute(start, SP, [(i + 1, i) for i in range(63)])
    bias = call(
        functools.partial(bias_body, 512),
        shape((2, 2, 3, 128, 128), F32),
        [pltpu.VMEM((15, 4, 32, 128), F32)],
        flops=10**8,
    )(table)
    att, away, w_near = call(
        attend_body,
        (shape((128, 256), BF), shape((128, 256), BF), shape((256, D), BF)),
        [
            pltpu.VMEM((256, 256), BF),
            pltpu.VMEM((2, 2, 128, 256), BF),
            pltpu.VMEM((2, 2, 3, 128, 128), F32),
            pltpu.SemaphoreType.DMA((5,)),
        ],
        flops=10**9,
        in_specs=[HBM_SPEC, VMEM_SPEC, HBM_SPEC, HBM_SPEC, VMEM_SPEC, HBM_SPEC, VMEM_SPEC, HBM_SPEC],
        out_specs=[VMEM_SPEC] * 3,
    )(in_hbm(q), prev, in_hbm(head), in_hbm(tail), nxt, in_hbm(bias), ctx_all, in_hbm(w_out))
    other = lax.ppermute(away, "c", SWAP)
    own = call(out_own_body, shape((128, D), F32), flops=10**9)(att, w_near)
    parts = call(out_proj_body, shape((4, 32, D), BF), flops=10**9)(own, other, w_pair)
    arrived = exchange(parts, "x")
    return call(final_body, shape((32, D), BF))(arrived, latent, gate)


def solution(mesh):
    torus = Mesh(mesh.devices.reshape(8, 2, 4, 4, 2), ALL)
    return jax.shard_map(
        on_device,
        mesh=torus,
        in_specs=(
            P(ALL, None),
            P(SP, None),
            P(),
            P(),
            P(),
            P(SP, TP),
            P(SP, TP),
            P(SP, TP),
            P(None, TP),
            P(None, TP),
            P(None, TP),
            P(TP, None),
            P(),
        ),
        out_specs=P(ALL, None),
        check_vma=False,
    )
```
